32 devices in a mesh: sp: 8 (over z, x), tp: 4 (over y, core).
Axes of the slice: x: 2, y: 2, z: 4, core: 2. Of those that a mesh axis runs over, the one named last changes fastest.
Arguments:
- latent: bfloat16 [6144, 2048], P(('sp', 'tp')), may hold values from -6 to 6
- context: bfloat16 [1024, 2048], P('sp'), may hold values from -6 to 6
- conditioning: float32 [2, 2048], replicated, may hold values from -6 to 6
- norm_gain: float32 [2048], replicated, may hold values from 0.1 to 1.9
- mod_shift: bfloat16 [2048, 2048], P('sp', 'tp'), may hold values from -0.1875 to 0.1875
- mod_scale: bfloat16 [2048, 2048], P('sp', 'tp'), may hold values from -0.1875 to 0.1875
- mod_gate: bfloat16 [2048, 2048], P('sp', 'tp'), may hold values from -0.1875 to 0.1875
- w_query: bfloat16 [2048, 2048], P(None, 'tp'), may hold values from -4 to 4
- w_key: bfloat16 [2048, 2048], P(None, 'tp'), may hold values from -0.125 to 0.125
- w_value: bfloat16 [2048, 2048], P(None, 'tp'), may hold values from -0.125 to 0.125
- w_out: bfloat16 [2048, 2048], P('tp'), may hold values from -0.125 to 0.125
- lambdas: float32 [16], P('tp'), may hold values from 0.3 to 0.8
- context_bias: float32 [16], P('tp'), may hold values from 0.8 to 2.2
- head_gain: float32 [128], replicated, may hold values from 0.1 to 1.9
Outputs:
- updated: bfloat16 [6144, 2048], P(('sp', 'tp'))
The draws below stay inside these ranges and needn't reach their ends.
All inputs are finite; a program needn't handle non-finite values.
Results may differ from the reference program's by a relative error of at most 0.01.
The reference program's roundings to bfloat16 on the way count: a program that leaves them out, or rounds other values in their place, can miss the bound.
Values may be sent and summed in bfloat16 or wider, within the bound.
No kernel may reach another device: no remote copies, remote signals or barrier semaphores. Data moves between devices by JAX's collectives and lax.ppermute only.
A program may use at most 128 MiB of HBM per device.

```python
import math
import jax
import jax.numpy as jnp
from jax import lax

D = 2048
HEADS = 16
HD = 64
CTX = 1024
TOKENS = 6144
N_TP = 4


def draw_w_query(key, part):
    entries = jnp.clip(jax.random.normal(key, (D, HEADS * 2 * HD), jnp.float32), -6.0, 6.0) * D ** (-0.5)
    return jnp.clip(entries, -4.0, 4.0).astype(jnp.bfloat16)


def steps_of(stream_key, extent, cuts, low, high):
    def one(axis_at, shards_of):
        heights = jax.random.uniform(jax.random.fold_in(jax.random.fold_in(stream_key, 6), axis_at), (shards_of,), jnp.float32, low / len(cuts), high / len(cuts))
        return jnp.repeat(jnp.exp(heights), extent[axis_at] // shards_of).reshape((-1,) + (1,) * (len(extent) - axis_at - 1))

    loudness = one(*cuts[0])
    for cut in cuts[1:]:
        loudness = loudness * one(*cut)
    return loudness


def noise(rng, shape, spread, bound, split=(), kind=jnp.bfloat16):
    loudness = steps_of(rng, shape, split, -0.22, 0.18) if split else 1.0
    values = jax.random.normal(rng, shape, jnp.float32) * spread * loudness
    return jnp.minimum(jnp.maximum(values, -bound), bound).astype(kind)


def setup_inputs(seed: int = 0) -> dict:
    key_list = jax.random.split(jax.random.key(seed), 15)
    latent = noise(key_list[0], (TOKENS, D), 1.0, 6.0, ((0, 32),))
    context = noise(key_list[1], (CTX, D), 1.0, 6.0, ((0, 8),))
    conditioning = noise(key_list[2], (2, D), 1.0, 6.0, (), jnp.float32)
    norm_gain = jnp.clip(1.0 + 0.18 * jax.random.normal(key_list[3], (D,), jnp.float32), 0.1, 1.9)
    mod_shift = noise(key_list[4], (D, D), (D // 2) ** -0.5, 0.1875, ((0, 8), (1, 4)))
    mod_scale = noise(key_list[5], (D, D), (D // 2) ** -0.5, 0.1875, ((0, 8), (1, 4)))
    mod_gate = noise(key_list[6], (D, D), (D // 2) ** -0.5, 0.1875, ((0, 8), (1, 4)))
    w_query = draw_w_query(jax.random.fold_in(key_list[14], 71), 0)
    w_key = noise(key_list[8], (D, HEADS * 2 * HD), D ** -0.5, 0.125, ((1, 4),))
    w_value = noise(key_list[9], (D, HEADS * 2 * HD), D ** -0.5, 0.125, ((1, 4),))
    w_out = noise(key_list[10], (HEADS * 2 * HD, D), (HEADS * 2 * HD) ** -0.5, 0.125, ((0, 4),))
    lambdas = jnp.clip(0.3 + 0.5 * jax.random.uniform(key_list[11], (HEADS,), jnp.float32) ** steps_of(key_list[11], (HEADS,), ((0, 4),), -0.2, 0.2), 0.3, 0.8)
    context_bias = jnp.clip(0.8 + 1.40000004 * jax.random.uniform(key_list[12], (HEADS,), jnp.float32) ** steps_of(key_list[12], (HEADS,), ((0, 4),), -0.2, 0.2), 0.8, 2.2)
    head_gain = jnp.clip(1.0 + 0.18 * jax.random.normal(key_list[13], (2 * HD,), jnp.float32), 0.1, 1.9)
    return dict(latent=latent, context=context, conditioning=conditioning, norm_gain=norm_gain, mod_shift=mod_shift, mod_scale=mod_scale, mod_gate=mod_gate, w_query=w_query, w_key=w_key, w_value=w_value, w_out=w_out, lambdas=lambdas, context_bias=context_bias, head_gain=head_gain)


EPS = 1e-06

def modulated(inputs, norm_scale, offset_vec, scale_vec):
    rows_float = inputs.astype(jnp.float32)
    normal = rows_float * lax.rsqrt(lax.optimization_barrier(jnp.mean(rows_float * rows_float, axis=-1, keepdims=True)) + EPS)
    return (normal * norm_scale * (1.0 + scale_vec) + offset_vec).astype(jnp.bfloat16)

def reference(latent, context, conditioning, norm_gain, mod_shift, mod_scale, mod_gate, w_query, w_key, w_value, w_out, lambdas, context_bias, head_gain):
    activated = jax.nn.silu(conditioning).astype(jnp.bfloat16)
    shifts = jnp.dot(activated, mod_shift, preferred_element_type=jnp.float32)
    scales = jnp.dot(activated, mod_scale, preferred_element_type=jnp.float32)
    gates = jnp.dot(activated, mod_gate, preferred_element_type=jnp.float32)
    hidden = modulated(latent, norm_gain, shifts[0], scales[0])
    hidden_context = modulated(context, norm_gain, shifts[1], scales[1])
    latent_len = latent.shape[0]
    context_len = context.shape[0]
    keys_len = latent_len + context_len
    queries = jnp.dot(hidden, w_query, preferred_element_type=jnp.float32).astype(jnp.bfloat16).reshape(latent_len, HEADS, 2, HD)
    both_rows = jnp.concatenate([hidden_context, hidden], axis=0)
    keys = jnp.dot(both_rows, w_key, preferred_element_type=jnp.float32).astype(jnp.bfloat16).reshape(keys_len, HEADS, 2, HD)
    values = jnp.dot(both_rows, w_value, preferred_element_type=jnp.float32).astype(jnp.bfloat16).reshape(keys_len, HEADS, 2 * HD)
    context_flags = (jnp.arange(keys_len, dtype=jnp.int32) < context_len).astype(jnp.float32)
    block_len = math.gcd(latent_len, 512)

    def per_head(operands):
        query_head, key_head, value_head, lambda_head, bias_head = operands
        biases = bias_head * context_flags
        key_float = key_head.astype(jnp.float32)

        def per_block(query_block):
            query_float = query_block.astype(jnp.float32)
            per_map = []
            for which_map in range(2):
                scores = jnp.einsum('qd,kd->qk', query_float[:, which_map], key_float[:, which_map]) * HD ** (-0.5) + biases[None, :]
                peak = lax.optimization_barrier(jnp.max(scores, axis=1, keepdims=True))
                raised = jnp.exp(scores - peak)
                totals = lax.optimization_barrier(jnp.sum(raised, axis=1, keepdims=True))
                weighted = jnp.dot(raised.astype(jnp.bfloat16), value_head, preferred_element_type=jnp.float32)
                per_map.append(weighted / totals)
            return per_map[0] - lambda_head * per_map[1]
        blocks = query_head.reshape(latent_len // block_len, block_len, 2, HD)
        return lax.map(per_block, blocks).reshape(latent_len, 2 * HD)
    mixed = lax.map(per_head, (jnp.moveaxis(queries, 1, 0), jnp.moveaxis(keys, 1, 0), jnp.moveaxis(values, 1, 0), lambdas, context_bias))
    normed = mixed * lax.rsqrt(lax.optimization_barrier(jnp.mean(mixed * mixed, axis=-1, keepdims=True)) + EPS) * head_gain
    flattened = jnp.moveaxis(normed, 0, 1).reshape(latent_len, HEADS * 2 * HD).astype(jnp.bfloat16)
    group_cols = HEADS * 2 * HD // N_TP
    summed = jnp.zeros((latent_len, w_out.shape[1]), jnp.float32)
    for group_index in range(N_TP):
        lower = group_index * group_cols
        partial_value = jnp.dot(flattened[:, lower:lower + group_cols], w_out[lower:lower + group_cols], preferred_element_type=jnp.float32).astype(jnp.bfloat16)
        partial_value = lax.optimization_barrier(partial_value)
        summed = summed + partial_value.astype(jnp.float32)
    attended = summed.astype(jnp.bfloat16)
    return (latent.astype(jnp.float32) + gates[0] * attended.astype(jnp.float32)).astype(jnp.bfloat16)
```

```python
import functools
import math

import jax
import jax.numpy as jnp
from jax import lax
from jax.experimental import pallas as pl
from jax.experimental.pallas import tpu as pltpu
from jax.sharding import Mesh
from jax.sharding import PartitionSpec as P

EPS = 1e-06
LOG2E = 1.4426950408889634
NT = (((1,), (1,)), ((), ()))
VMEM_LIMIT = 60 * 1024 * 1024


def params(*semantics):
    return pltpu.CompilerParams(dimension_semantics=semantics, vmem_limit_bytes=VMEM_LIMIT)


def whole_spec(shape):
    return pl.BlockSpec(shape, lambda i: (0,) * len(shape))


def project_kernel(ctx, heads, width, lat_ref, ctx_ref, mod_ref, wq_ref, wk_ref, wv_ref, q_ref, kv_ref, hid_ref):
    @pl.when(pl.program_id(0) == 0)
    def _():
        def norm(src_ref, which, start, rows):
            x = src_ref[pl.ds(start, rows), :].astype(jnp.float32)
            inv = lax.rsqrt(jnp.mean(x * x, axis=-1, keepdims=True) + EPS)
            out = x * inv * mod_ref[which, 0:1, :] + mod_ref[which, 1:2, :]
            return out.astype(jnp.bfloat16)

        step = math.gcd(ctx, 64)

        def ctx_body(i, carry):
            hid_ref[pl.ds(pl.multiple_of(i * step, step), step), :] = norm(
                ctx_ref, 1, pl.multiple_of(i * step, step), step
            )
            return carry

        lax.fori_loop(0, ctx // step, ctx_body, 0)
        lat = lat_ref.shape[0]
        lstep = math.gcd(lat, 64)

        def lat_body(i, carry):
            at = pl.multiple_of(i * lstep, lstep)
            hid_ref[pl.ds(ctx + at, lstep), :] = norm(lat_ref, 0, at, lstep)
            return carry

        lax.fori_loop(0, lat // lstep, lat_body, 0)

    hidden = hid_ref[...]
    q = jnp.dot(hidden[ctx:], wq_ref[...], preferred_element_type=jnp.float32).astype(jnp.bfloat16)
    k = jnp.dot(hidden, wk_ref[...], preferred_element_type=jnp.float32).astype(jnp.bfloat16)
    v = jnp.dot(hidden, wv_ref[...], preferred_element_type=jnp.float32).astype(jnp.bfloat16)
    for h in range(heads):
        cols = slice(h * width, (h + 1) * width)
        q_ref[h] = q[:, cols]
        kv_ref[h, :, :width] = k[:, cols]
        kv_ref[h, :, width:] = v[:, cols]


def project(latent, context, mods, w_query, w_key, w_value, head_count, width):
    lat, dim = latent.shape
    ctx = context.shape[0]
    per = 2 if head_count % 2 == 0 else 1
    weight = pl.BlockSpec((dim, per * width), lambda i: (0, i))
    return pl.pallas_call(
        functools.partial(project_kernel, ctx, per, width),
        grid=(head_count // per,),
        in_specs=[
            whole_spec((lat, dim)),
            whole_spec((ctx, dim)),
            whole_spec(mods.shape),
            weight,
            weight,
            weight,
        ],
        out_specs=[
            pl.BlockSpec((per, lat, width), lambda i: (i, 0, 0)),
            pl.BlockSpec((per, ctx + lat, 2 * width), lambda i: (i, 0, 0)),
        ],
        out_shape=[
            jax.ShapeDtypeStruct((head_count, lat, width), jnp.bfloat16),
            jax.ShapeDtypeStruct((head_count, ctx + lat, 2 * width), jnp.bfloat16),
        ],
        scratch_shapes=[pltpu.VMEM((ctx + lat, dim), jnp.bfloat16)],
        compiler_params=params("arbitrary"),
        cost_estimate=pl.CostEstimate(
            flops=6 * (ctx + lat) * dim * head_count * width,
            bytes_accessed=2 * dim * (lat + ctx + 3 * head_count * width),
            transcendentals=0,
        ),
        name="project",
    )(latent, context, mods, w_query, w_key, w_value)


def attend_kernel(ctx, first, last, *refs):
    refs = list(refs)
    scal_ref, q_ref, kv_ref = refs[:3]
    at = 3
    if not first:
        ml_in, acc_in = refs[at : at + 2]
        at += 2
    if last:
        gain_ref, out_ref = refs[at : at + 2]
    else:
        ml_out, acc_out = refs[at : at + 2]
    rows, width = q_ref.shape
    sources, keys = kv_ref.shape[0], kv_ref.shape[1]
    half = width // 2
    scaled = q_ref[...].astype(jnp.float32) * (half ** (-0.5) * LOG2E)
    high = scaled.astype(jnp.bfloat16)
    low = (scaled - high.astype(jnp.float32)).astype(jnp.bfloat16)
    lanes = lax.broadcasted_iota(jnp.int32, (rows, width), 1)
    zero = jnp.zeros_like(high)
    bias = scal_ref[1]
    if ctx % 128:
        flags = lax.broadcasted_iota(jnp.int32, (1, keys), 1) < ctx
        bias_row = jnp.where(flags, bias, 0.0)
    sides = []
    for which in range(2):
        keep = (lanes < half) if which == 0 else (lanes >= half)
        sides.append(
            jnp.concatenate([jnp.where(keep, high, zero), jnp.where(keep, low, zero)], axis=1)
        )
    state = []
    for which in range(2):
        if first:
            state.append(None)
        else:
            ml = ml_in[which]
            state.append((ml[:, 0:1], ml[:, half : half + 1], acc_in[which]))
    for source in range(sources):
        k = kv_ref[source, :, :width]
        v = kv_ref[source, :, width:]
        doubled = jnp.concatenate([k, k], axis=1)
        for which in range(2):
            s = lax.dot_general(sides[which], doubled, NT, preferred_element_type=jnp.float32)
            if ctx % 128:
                s = s + bias_row
            else:
                s = jnp.concatenate([s[:, :ctx] + bias, s[:, ctx:]], axis=1)
            top = jnp.max(s, axis=1, keepdims=True)
            if state[which] is None:
                p = jnp.exp2(s - top)
                total = jnp.sum(p, axis=1, keepdims=True)
                acc = jnp.dot(p.astype(jnp.bfloat16), v, preferred_element_type=jnp.float32)
            else:
                old, total, acc = state[which]
                top = jnp.maximum(old, top)
                fade = jnp.exp2(old - top)
                p = jnp.exp2(s - top)
                total = total * fade + jnp.sum(p, axis=1, keepdims=True)
                acc = acc * fade + jnp.dot(
                    p.astype(jnp.bfloat16), v, preferred_element_type=jnp.float32
                )
            state[which] = (top, total, acc)
    if last:
        mixed = state[0][2] / state[0][1] - scal_ref[0] * (state[1][2] / state[1][1])
        normed = mixed * lax.rsqrt(jnp.mean(mixed * mixed, axis=-1, keepdims=True) + EPS)
        out_ref[...] = (normed * gain_ref[...]).astype(jnp.bfloat16)
    else:
        for which in range(2):
            top, total, acc = state[which]
            ml_out[which] = jnp.where(lanes < half, top, total)
            acc_out[which] = acc


def attend(ctx, scalars, queries, kv, carried, gain, last):
    tokens, width = queries.shape
    block = math.gcd(tokens, 256)
    first = carried is None
    row_spec = pl.BlockSpec((block, width), lambda i: (i, 0))
    state_spec = pl.BlockSpec((2, block, width), lambda i: (0, i, 0))
    in_specs = [pl.BlockSpec(memory_space=pltpu.SMEM), row_spec, whole_spec(kv.shape)]
    operands = [scalars, queries, kv]
    if not first:
        in_specs += [state_spec, state_spec]
        operands += list(carried)
    if last:
        in_specs.append(whole_spec((1, width)))
        operands.append(gain)
        out_specs = row_spec
        out_shape = jax.ShapeDtypeStruct((tokens, width), jnp.bfloat16)
    else:
        out_specs = [state_spec, state_spec]
        out_shape = [jax.ShapeDtypeStruct((2, tokens, width), jnp.float32)] * 2
    key_count = kv.shape[0] * kv.shape[1]
    return pl.pallas_call(
        functools.partial(attend_kernel, ctx, first, last),
        grid=(tokens // block,),
        in_specs=in_specs,
        out_specs=out_specs,
        out_shape=out_shape,
        compiler_params=params("arbitrary"),
        cost_estimate=pl.CostEstimate(
            flops=16 * tokens * key_count * width,
            bytes_accessed=2 * key_count * 2 * width + 8 * tokens * width,
            transcendentals=2 * tokens * key_count,
        ),
        name="attend",
    )(*operands)


def finish_kernel(head_count, groups, recv_ref, w_ref, lat_ref, gate_ref, out_ref):
    rows_w = w_ref.shape[0] // groups
    summed = None
    for t in range(groups):
        left = jnp.concatenate([recv_ref[a * groups + t] for a in range(head_count)], axis=1)
        part = jnp.dot(
            left, w_ref[t * rows_w : (t + 1) * rows_w, :], preferred_element_type=jnp.float32
        ).astype(jnp.bfloat16)
        part = part.astype(jnp.float32)
        summed = part if summed is None else summed + part
    attended = summed.astype(jnp.bfloat16).astype(jnp.float32)
    out_ref[...] = (lat_ref[...].astype(jnp.float32) + gate_ref[...] * attended).astype(jnp.bfloat16)


def finish(recv, w_full, latent, gate, head_count, groups):
    rows, dim = latent.shape
    block = math.gcd(dim, 512)
    return pl.pallas_call(
        functools.partial(finish_kernel, head_count, groups),
        grid=(dim // block,),
        in_specs=[
            whole_spec(recv.shape),
            pl.BlockSpec((w_full.shape[0], block), lambda i: (0, i)),
            pl.BlockSpec((rows, block), lambda i: (0, i)),
            pl.BlockSpec((1, block), lambda i: (0, i)),
        ],
        out_specs=pl.BlockSpec((rows, block), lambda i: (0, i)),
        out_shape=jax.ShapeDtypeStruct((rows, dim), jnp.bfloat16),
        compiler_params=params("arbitrary"),
        cost_estimate=pl.CostEstimate(
            flops=2 * rows * dim * w_full.shape[0],
            bytes_accessed=2 * dim * w_full.shape[0],
            transcendentals=0,
        ),
        name="finish",
    )(recv, w_full, latent, gate)


def per_device(
    latent,
    context,
    conditioning,
    norm_gain,
    mod_shift,
    mod_scale,
    mod_gate,
    w_query,
    w_key,
    w_value,
    w_out,
    lambdas,
    context_bias,
    head_gain,
):
    width = head_gain.shape[0]
    head_count = lambdas.shape[0]
    parts = lax.axis_size("part")
    tp = lax.axis_size("tp")
    ctx = context.shape[0]
    rows_sp = mod_shift.shape[0]
    sp_at = lax.axis_index(("head", "part"))
    cond_rows = lax.dynamic_slice_in_dim(conditioning, sp_at * rows_sp, rows_sp, 1)
    activated = jax.nn.silu(cond_rows).astype(jnp.bfloat16)
    partials = jnp.concatenate(
        [
            jnp.dot(activated, matrix, preferred_element_type=jnp.float32)
            for matrix in (mod_shift, mod_scale, mod_gate)
        ],
        axis=0,
    )
    gathered = lax.all_gather(partials, ("head", "part", "tp"), axis=0)
    summed = jnp.sum(gathered.reshape(-1, tp, 3, 2, partials.shape[1]), axis=0)
    modulation = jnp.moveaxis(summed, 0, 2).reshape(3, 2, -1)
    factors = norm_gain * (1.0 + modulation[1])
    mods = jnp.stack([factors, modulation[0]], axis=1)
    rows = lax.all_gather(latent, "tp", axis=0, tiled=True)
    w_full = lax.all_gather(w_out, "tp", axis=0, tiled=True)
    queries, kv = project(rows, context, mods, w_query, w_key, w_value, head_count, width)
    kv = lax.all_to_all(kv, "head", 0, 0, tiled=True)
    remote = [
        lax.ppermute(kv, "part", [(i, (i - j) % parts) for i in range(parts)])
        for j in range(1, parts)
    ]
    queries = lax.all_to_all(queries, "head", 0, 0, tiled=True)
    queries = queries.reshape(-1, width)
    head_at = lax.axis_index("head")
    scalars = jnp.stack([lambdas[head_at], context_bias[head_at] * LOG2E])
    gain = head_gain.reshape(1, width)
    carried = None
    blocks = [kv] + remote
    for j, block in enumerate(blocks):
        carried = attend(ctx, scalars, queries, block, carried, gain, j == len(blocks) - 1)
    normed = carried.reshape(head_count * tp, latent.shape[0], width)
    recv = lax.all_to_all(normed, ("head", "tp"), 0, 0, tiled=True)
    return finish(recv, w_full, latent, modulation[2, 0:1], head_count, tp)


def solution(mesh):
    sp, tp = mesh.shape["sp"], mesh.shape["tp"]

    def run(*args):
        head_count = args[11].shape[0] // tp
        inner = Mesh(mesh.devices.reshape(head_count, sp // head_count, tp), ("head", "part", "tp"))
        seq = ("head", "part")
        every = ("head", "part", "tp")
        return jax.shard_map(
            per_device,
            mesh=inner,
            in_specs=(
                P(every, None),
                P(seq, None),
                P(),
                P(),
                P(seq, "tp"),
                P(seq, "tp"),
                P(seq, "tp"),
                P(None, "tp"),
                P(None, "tp"),
                P(None, "tp"),
                P("tp", None),
                P("tp"),
                P("tp"),
                P(),
            ),
            out_specs=P(every, None),
            check_vma=False,
        )(*args)

    return run
```

```python
import functools
import math

import jax
import jax.numpy as jnp
from jax import lax
from jax.experimental import pallas as pl
from jax.experimental.pallas import tpu as pltpu
from jax.sharding import Mesh
from jax.sharding import PartitionSpec as P

EPS = 1e-06
LOG2E = 1.4426950408889634
NT = (((1,), (1,)), ((), ()))
VMEM_LIMIT = 60 * 1024 * 1024


def params(*semantics):
    return pltpu.CompilerParams(dimension_semantics=semantics, vmem_limit_bytes=VMEM_LIMIT)


def whole_spec(shape):
    return pl.BlockSpec(shape, lambda i: (0,) * len(shape))


def project_kernel(ctx, heads, width, lat_ref, ctx_ref, mod_ref, wq_ref, wk_ref, wv_ref, q_ref, kv_ref, hid_ref):
    @pl.when(pl.program_id(0) == 0)
    def _():
        def norm(src_ref, which, start, rows):
            x = src_ref[pl.ds(start, rows), :].astype(jnp.float32)
            inv = lax.rsqrt(jnp.mean(x * x, axis=-1, keepdims=True) + EPS)
            out = x * inv * mod_ref[which, 0:1, :] + mod_ref[which, 1:2, :]
            return out.astype(jnp.bfloat16)

        step = math.gcd(ctx, 64)

        def ctx_body(i, carry):
            hid_ref[pl.ds(pl.multiple_of(i * step, step), step), :] = norm(
                ctx_ref, 1, pl.multiple_of(i * step, step), step
            )
            return carry

        lax.fori_loop(0, ctx // step, ctx_body, 0)
        lat = lat_ref.shape[0]
        lstep = math.gcd(lat, 64)

        def lat_body(i, carry):
            at = pl.multiple_of(i * lstep, lstep)
            hid_ref[pl.ds(ctx + at, lstep), :] = norm(lat_ref, 0, at, lstep)
            return carry

        lax.fori_loop(0, lat // lstep, lat_body, 0)

    hidden = hid_ref[...]
    q = jnp.dot(hidden[ctx:], wq_ref[...], preferred_element_type=jnp.float32).astype(jnp.bfloat16)
    k = jnp.dot(hidden, wk_ref[...], preferred_element_type=jnp.float32).astype(jnp.bfloat16)
    v = jnp.dot(hidden, wv_ref[...], preferred_element_type=jnp.float32).astype(jnp.bfloat16)
    for h in range(heads):
        cols = slice(h * width, (h + 1) * width)
        q_ref[h] = q[:, cols]
        kv_ref[h, :, :width] = k[:, cols]
        kv_ref[h, :, width:] = v[:, cols]


def project(latent, context, mods, w_query, w_key, w_value, head_count, width):
    lat, dim = latent.shape
    ctx = context.shape[0]
    per = 2 if head_count % 2 == 0 else 1
    weight = pl.BlockSpec((dim, per * width), lambda i: (0, i))
    return pl.pallas_call(
        functools.partial(project_kernel, ctx, per, width),
        grid=(head_count // per,),
        in_specs=[
            whole_spec((lat, dim)),
            whole_spec((ctx, dim)),
            whole_spec(mods.shape),
            weight,
            weight,
            weight,
        ],
        out_specs=[
            pl.BlockSpec((per, lat, width), lambda i: (i, 0, 0)),
            pl.BlockSpec((per, ctx + lat, 2 * width), lambda i: (i, 0, 0)),
        ],
        out_shape=[
            jax.ShapeDtypeStruct((head_count, lat, width), jnp.bfloat16),
            jax.ShapeDtypeStruct((head_count, ctx + lat, 2 * width), jnp.bfloat16),
        ],
        scratch_shapes=[pltpu.VMEM((ctx + lat, dim), jnp.bfloat16)],
        compiler_params=params("arbitrary"),
        cost_estimate=pl.CostEstimate(
            flops=6 * (ctx + lat) * dim * head_count * width,
            bytes_accessed=2 * dim * (lat + ctx + 3 * head_count * width),
            transcendentals=0,
        ),
        name="project",
    )(latent, context, mods, w_query, w_key, w_value)


def attend_kernel(ctx, first, last, sources, *refs):
    refs = list(refs)
    scal_ref, q_ref = refs[:2]
    kv_refs = refs[2 : 2 + sources]
    at = 2 + sources
    if not first:
        ml_in, acc_in = refs[at : at + 2]
        at += 2
    if last:
        gain_ref, out_ref = refs[at : at + 2]
    else:
        ml_out, acc_out = refs[at : at + 2]
    rows, width = q_ref.shape
    keys = kv_refs[0].shape[0]
    half = width // 2
    scaled = q_ref[...].astype(jnp.float32) * (half ** (-0.5) * LOG2E)
    high = scaled.astype(jnp.bfloat16)
    low = (scaled - high.astype(jnp.float32)).astype(jnp.bfloat16)
    lanes = lax.broadcasted_iota(jnp.int32, (rows, width), 1)
    zero = jnp.zeros_like(high)
    bias = scal_ref[1]
    if ctx % 128:
        flags = lax.broadcasted_iota(jnp.int32, (1, keys), 1) < ctx
        bias_row = jnp.where(flags, bias, 0.0)
    sides = []
    for which in range(2):
        keep = (lanes < half) if which == 0 else (lanes >= half)
        sides.append(
            jnp.concatenate([jnp.where(keep, high, zero), jnp.where(keep, low, zero)], axis=1)
        )
    state = []
    for which in range(2):
        if first:
            state.append(None)
        else:
            ml = ml_in[which]
            state.append((ml[:, 0:1], ml[:, half : half + 1], acc_in[which]))
    def products(kv_ref):
        k = kv_ref[:, :width]
        doubled = jnp.concatenate([k, k], axis=1)
        return [
            lax.dot_general(side, doubled, NT, preferred_element_type=jnp.float32)
            for side in sides
        ]

    ahead = products(kv_refs[0])
    for source, kv_ref in enumerate(kv_refs):
        dots = ahead
        if source + 1 < sources:
            ahead = products(kv_refs[source + 1])
        v = kv_ref[:, width:]
        v = jnp.concatenate([v, jnp.ones_like(v)], axis=1)
        for which in range(2):
            s = dots[which]
            if ctx % 128:
                s = s + bias_row
            else:
                s = jnp.concatenate([s[:, :ctx] + bias, s[:, ctx:]], axis=1)
            top = jnp.max(s, axis=1, keepdims=True)
            if state[which] is None:
                p = jnp.exp2(s - top)
                acc = jnp.dot(p.astype(jnp.bfloat16), v, preferred_element_type=jnp.float32)
                total = acc[:, width:]
                acc = acc[:, :width]
            else:
                old, total, acc = state[which]
                top = jnp.maximum(old, top)
                fade = jnp.exp2(old - top)
                p = jnp.exp2(s - top)
                part = jnp.dot(p.astype(jnp.bfloat16), v, preferred_element_type=jnp.float32)
                total = total * fade + part[:, width:]
                acc = acc * fade + part[:, :width]
            state[which] = (top, total, acc)
    if last:
        mixed = state[0][2] / state[0][1] - scal_ref[0] * (state[1][2] / state[1][1])
        normed = mixed * lax.rsqrt(jnp.mean(mixed * mixed, axis=-1, keepdims=True) + EPS)
        out_ref[...] = (normed * gain_ref[...]).astype(jnp.bfloat16)
    else:
        for which in range(2):
            top, total, acc = state[which]
            ml_out[which] = jnp.where(lanes < half, top, total)
            acc_out[which] = acc


def attend(ctx, scalars, queries, wave, carried, gain, last):
    tokens, width = queries.shape
    block = math.gcd(tokens, 512)
    first = carried is None
    row_spec = pl.BlockSpec((block, width), lambda i: (i, 0))
    state_spec = pl.BlockSpec((2, block, width), lambda i: (0, i, 0))
    in_specs = [pl.BlockSpec(memory_space=pltpu.SMEM), row_spec]
    in_specs += [whole_spec(kv.shape) for kv in wave]
    operands = [scalars, queries, *wave]
    if not first:
        in_specs += [state_spec, state_spec]
        operands += list(carried)
    if last:
        in_specs.append(whole_spec((1, width)))
        operands.append(gain)
        out_specs = row_spec
        out_shape = jax.ShapeDtypeStruct((tokens, width), jnp.bfloat16)
    else:
        out_specs = [state_spec, state_spec]
        out_shape = [jax.ShapeDtypeStruct((2, tokens, width), jnp.float32)] * 2
    key_count = sum(kv.shape[0] for kv in wave)
    return pl.pallas_call(
        functools.partial(attend_kernel, ctx, first, last, len(wave)),
        grid=(tokens // block,),
        in_specs=in_specs,
        out_specs=out_specs,
        out_shape=out_shape,
        compiler_params=params("arbitrary"),
        cost_estimate=pl.CostEstimate(
            flops=16 * tokens * key_count * width,
            bytes_accessed=2 * key_count * 2 * width + 8 * tokens * width,
            transcendentals=2 * tokens * key_count,
        ),
        name="attend",
    )(*operands)


def finish_kernel(head_count, groups, recv_ref, w_ref, lat_ref, gate_ref, out_ref):
    rows_w = w_ref.shape[0] // groups
    summed = None
    for t in range(groups):
        left = jnp.concatenate([recv_ref[a * groups + t] for a in range(head_count)], axis=1)
        part = jnp.dot(
            left, w_ref[t * rows_w : (t + 1) * rows_w, :], preferred_element_type=jnp.float32
        ).astype(jnp.bfloat16)
        part = part.astype(jnp.float32)
        summed = part if summed is None else summed + part
    attended = summed.astype(jnp.bfloat16).astype(jnp.float32)
    out_ref[...] = (lat_ref[...].astype(jnp.float32) + gate_ref[...] * attended).astype(jnp.bfloat16)


def finish(recv, w_full, latent, gate, head_count, groups):
    rows, dim = latent.shape
    block = math.gcd(dim, 512)
    return pl.pallas_call(
        functools.partial(finish_kernel, head_count, groups),
        grid=(dim // block,),
        in_specs=[
            whole_spec(recv.shape),
            pl.BlockSpec((w_full.shape[0], block), lambda i: (0, i)),
            pl.BlockSpec((rows, block), lambda i: (0, i)),
            pl.BlockSpec((1, block), lambda i: (0, i)),
        ],
        out_specs=pl.BlockSpec((rows, block), lambda i: (0, i)),
        out_shape=jax.ShapeDtypeStruct((rows, dim), jnp.bfloat16),
        compiler_params=params("arbitrary"),
        cost_estimate=pl.CostEstimate(
            flops=2 * rows * dim * w_full.shape[0],
            bytes_accessed=2 * dim * w_full.shape[0],
            transcendentals=0,
        ),
        name="finish",
    )(recv, w_full, latent, gate)


def per_device(
    latent,
    context,
    conditioning,
    norm_gain,
    mod_shift,
    mod_scale,
    mod_gate,
    w_query,
    w_key,
    w_value,
    w_out,
    lambdas,
    context_bias,
    head_gain,
):
    width = head_gain.shape[0]
    head_count = lambdas.shape[0]
    parts = lax.axis_size("part")
    tp = lax.axis_size("tp")
    ctx = context.shape[0]
    rows_sp = mod_shift.shape[0]
    sp_at = lax.axis_index(("head", "part"))
    cond_rows = lax.dynamic_slice_in_dim(conditioning, sp_at * rows_sp, rows_sp, 1)
    activated = jax.nn.silu(cond_rows).astype(jnp.bfloat16)
    partials = jnp.concatenate(
        [
            jnp.dot(activated, matrix, preferred_element_type=jnp.float32)
            for matrix in (mod_shift, mod_scale, mod_gate)
        ],
        axis=0,
    )
    for axis in ("head", "part"):
        partials = jnp.sum(lax.all_gather(partials, axis, axis=0), axis=0)
    modulation = lax.all_gather(partials, "tp", axis=1, tiled=True).reshape(3, 2, -1)
    factors = norm_gain * (1.0 + modulation[1])
    mods = jnp.stack([factors, modulation[0]], axis=1)
    rows = lax.all_gather(latent, "tp", axis=0, tiled=True)
    w_full = lax.all_gather(w_out, "tp", axis=0, tiled=True)
    queries, kv = project(rows, context, mods, w_query, w_key, w_value, head_count, width)
    head_at = lax.axis_index("head")

    def across(block):
        return [
            lax.ppermute(block, "part", [(i, (i - j) % parts) for i in range(parts)])
            for j in range(1, parts)
        ]

    def kv_of(head):
        return lax.dynamic_index_in_dim(kv, head, 0, keepdims=False)

    own = kv_of(head_at)
    arrived = [
        lax.ppermute(
            kv_of(lax.rem(head_at + j, head_count)),
            "head",
            [(i, (i + j) % head_count) for i in range(head_count)],
        )
        for j in range(1, head_count)
    ]
    near = [own] + across(own)
    queries = lax.all_to_all(queries, "head", 0, 0, tiled=True)
    queries = queries.reshape(-1, width)
    scalars = jnp.stack([lambdas[head_at], context_bias[head_at] * LOG2E])
    gain = head_gain.reshape(1, width)
    rest = arrived and parts > 1
    carried = attend(ctx, scalars, queries, near, None, gain, not arrived)
    if arrived:
        arrived, carried = lax.optimization_barrier((arrived, carried))
        far = [block for one in arrived for block in across(one)]
        carried = attend(ctx, scalars, queries, arrived, carried, gain, not rest)
    if rest:
        carried = attend(ctx, scalars, queries, far, carried, gain, True)
    normed = carried.reshape(head_count * tp, latent.shape[0], width)
    recv = lax.all_to_all(normed, ("head", "tp"), 0, 0, tiled=True)
    return finish(recv, w_full, latent, modulation[2, 0:1], head_count, tp)


def solution(mesh):
    sp, tp = mesh.shape["sp"], mesh.shape["tp"]

    def run(*args):
        head_count = args[11].shape[0] // tp
        inner = Mesh(mesh.devices.reshape(head_count, sp // head_count, tp), ("head", "part", "tp"))
        seq = ("head", "part")
        every = ("head", "part", "tp")
        return jax.shard_map(
            per_device,
            mesh=inner,
            in_specs=(
                P(every, None),
                P(seq, None),
                P(),
                P(),
                P(seq, "tp"),
                P(seq, "tp"),
                P(seq, "tp"),
                P(None, "tp"),
                P(None, "tp"),
                P(None, "tp"),
                P("tp", None),
                P("tp"),
                P("tp"),
                P(),
            ),
            out_specs=P(every, None),
            check_vma=False,
        )(*args)

    return run
```
